256 devices in a mesh: sp: 64 (over z, x, core), tp: 4 (over y).
Axes of the slice: x: 4, y: 4, z: 8, core: 2. Of those that a mesh axis runs over, the one named last changes fastest.
Arguments:
- tokens: bfloat16 [65536, 2048], P('sp'), may hold values from -8 to 8
- norm_gain: float32 [2048], replicated, may hold values from 0.1 to 1.9
- query_weight: bfloat16 [2048, 512], P(None, 'tp'), may hold values from -40 to 40
- key_weight: bfloat16 [2048, 256], P(None, 'tp'), may hold values from -1 to 1
- value_weight: bfloat16 [2048, 256], P(None, 'tp'), may hold values from -0.125 to 0.125
- sink_logits: float32 [8], P('tp'), may hold values from 1 to 6
- conv_in_weight: bfloat16 [2048, 512], P(None, 'tp'), may hold values from -0.125 to 0.125
- conv_gate_weight: bfloat16 [2048, 512], P(None, 'tp'), may hold values from -0.125 to 0.125
- conv_taps: bfloat16 [31, 512], replicated, may hold values from -1 to 1
- conv_gain: float32 [512], replicated, may hold values from 0.1 to 1.9
- point_weight: bfloat16 [512, 512], replicated, may hold values from -0.25 to 0.25
- output_gain: float32 [1024], replicated, may hold values from 0.1 to 1.9
- output_weight: bfloat16 [1024, 2048], P('sp'), may hold values from -0.1875 to 0.1875
Outputs:
- mixed_output: bfloat16 [65536, 2048], P(('sp', 'tp'))
The draws below stay inside these ranges and needn't reach their ends.
All inputs are finite; a program needn't handle non-finite values.
Results may differ from the reference program's by a relative error of at most 0.0087.
Values may be sent and summed in bfloat16 or wider, within the bound.
A program may use at most 64 MiB of HBM per device.

```python
import jax
import jax.numpy as jnp
from jax import lax

D = 2048
HEADS = 8
KV_HEADS = 4
HEAD_DIM = 64
CHANNELS = 512
WINDOW = 128
CONV_WIDTH = 31
TOKENS = 65536
MIX = 1024


def base_query(key):
    gaussian = jax.random.normal(jax.random.fold_in(key, 501), (D, HEADS * HEAD_DIM), jnp.float32)
    return jnp.clip(gaussian, -6.0, 6.0) * D ** (-0.5)


def draw_query_weight(key, part):
    unscaled = base_query(key)
    return unscaled.astype(jnp.bfloat16)


def draw_key_weight(key, part):
    fresh_noise = jax.random.normal(jax.random.fold_in(key, 502), (D, KV_HEADS * HEAD_DIM), jnp.float32)
    fresh_noise = jnp.clip(fresh_noise, -6.0, 6.0) * D ** (-0.5)
    return fresh_noise.astype(jnp.bfloat16)


def draw_tokens(key, part):
    shape_rows = (TOKENS, D)
    gaussian = jnp.clip(jax.random.normal(jax.random.fold_in(key, 601), shape_rows, jnp.float32), -6.0, 6.0)
    return gaussian.astype(jnp.bfloat16)


def block_levels(key, extent, split, low, top_value):
    def one(dim, shards_of):
        heights = jax.random.uniform(jax.random.fold_in(jax.random.fold_in(key, 6), dim), (shards_of,), jnp.float32, low / len(split), top_value / len(split))
        return jnp.repeat(jnp.exp(heights), extent[dim] // shards_of).reshape((-1,) + (1,) * (len(extent) - dim - 1))

    factor_of = one(*split[0])
    for cut in split[1:]:
        factor_of = factor_of * one(*cut)
    return factor_of


def scatter_about(key, dims, deviation, reach, cuts=(), kind=jnp.bfloat16):
    entries = deviation * jax.random.normal(key, dims, jnp.float32)
    if cuts:
        entries = entries * block_levels(key, dims, cuts, -0.22, 0.18)
    return jnp.clip(entries, -reach, reach).astype(kind)


def setup_inputs(seed: int = 0) -> dict:
    seeds = jax.random.split(jax.random.key(seed), 14)
    return {
        "tokens": draw_tokens(jax.random.fold_in(seeds[13], 71), 0),
        "norm_gain": jnp.clip(1.0 + 0.18 * jax.random.normal(seeds[1], (D,), jnp.float32), 0.1, 1.9),
        "query_weight": draw_query_weight(jax.random.fold_in(seeds[13], 71), 0),
        "key_weight": draw_key_weight(jax.random.fold_in(seeds[13], 71), 0),
        "value_weight": scatter_about(seeds[4], (D, KV_HEADS * HEAD_DIM), D ** -0.5, 0.125, ((1, 4),)),
        "sink_logits": jnp.clip(1.0 + 5.0 * jax.random.uniform(seeds[5], (HEADS,), jnp.float32) ** block_levels(seeds[5], (HEADS,), ((0, 4),), -0.2, 0.2), 1.0, 6.0),
        "conv_in_weight": scatter_about(seeds[6], (D, CHANNELS), D ** -0.5, 0.125, ((1, 4),)),
        "conv_gate_weight": scatter_about(seeds[7], (D, CHANNELS), D ** -0.5, 0.125, ((1, 4),)),
        "conv_taps": scatter_about(seeds[8], (CONV_WIDTH, CHANNELS), CONV_WIDTH ** -0.5, 1.0),
        "conv_gain": jnp.clip(1.0 + 0.18 * jax.random.normal(seeds[9], (CHANNELS,), jnp.float32), 0.1, 1.9),
        "point_weight": scatter_about(seeds[10], (CHANNELS, CHANNELS), CHANNELS ** -0.5, 0.25),
        "output_gain": jnp.clip(1.0 + 0.18 * jax.random.normal(seeds[11], (MIX,), jnp.float32), 0.1, 1.9),
        "output_weight": scatter_about(seeds[12], (MIX, D), MIX ** -0.5, 0.1875, ((0, 64),)),
    }


NORM_EPSILON = 1e-06
MASKED_SCORE = -1e+30

def rms_rows(values, scale_gain):
    return values * lax.rsqrt(lax.optimization_barrier(jnp.mean(values * values, axis=-1, keepdims=True)) + NORM_EPSILON) * scale_gain

def depthwise(current, earlier_rows, tap_weights):
    extended = jnp.concatenate([earlier_rows, current], axis=0).astype(jnp.float32)
    tap_floats = tap_weights.astype(jnp.float32)
    row_count = current.shape[0]
    result = jnp.zeros(current.shape, jnp.float32)
    for tap_index in range(CONV_WIDTH):
        result = result + tap_floats[tap_index] * extended[tap_index:tap_index + row_count]
    return lax.optimization_barrier(result.astype(jnp.bfloat16))

def layer_activate(conv_rows, channel_gain):
    widened = conv_rows.astype(jnp.float32)
    centered = widened - lax.optimization_barrier(jnp.mean(widened, axis=-1, keepdims=True))
    scaled = centered * lax.rsqrt(lax.optimization_barrier(jnp.mean(centered * centered, axis=-1, keepdims=True)) + NORM_EPSILON) * channel_gain
    return jax.nn.silu(scaled).astype(jnp.bfloat16)

def merge_groups(attended, pointwise, output_gain):
    head_width = attended.shape[1]
    return jnp.concatenate([rms_rows(attended.astype(jnp.float32), output_gain[:head_width]), rms_rows(pointwise, output_gain[head_width:])], axis=1).astype(jnp.bfloat16)

def reference(tokens, norm_gain, query_weight, key_weight, value_weight, sink_logits, conv_in_weight, conv_gate_weight, conv_taps, conv_gain, point_weight, output_gain, output_weight):
    normed = rms_rows(tokens.astype(jnp.float32), norm_gain).astype(jnp.bfloat16)
    queries = jnp.dot(normed, query_weight, preferred_element_type=jnp.float32).astype(jnp.bfloat16)
    key_part = jnp.dot(normed, key_weight, preferred_element_type=jnp.float32).astype(jnp.bfloat16)
    value_part = jnp.dot(normed, value_weight, preferred_element_type=jnp.float32).astype(jnp.bfloat16)
    conv_in = jnp.dot(normed, conv_in_weight, preferred_element_type=jnp.float32)
    conv_gate = jnp.dot(normed, conv_gate_weight, preferred_element_type=jnp.float32)
    gated_rows = (conv_in * jax.nn.sigmoid(conv_gate)).astype(jnp.bfloat16)
    group_size = HEADS // KV_HEADS
    block_count = TOKENS // WINDOW
    head_queries = jnp.transpose(queries.reshape(TOKENS, KV_HEADS, group_size, HEAD_DIM), (1, 0, 2, 3))
    head_keys = jnp.transpose(key_part.reshape(TOKENS, KV_HEADS, HEAD_DIM), (1, 0, 2))
    head_values = jnp.transpose(value_part.reshape(TOKENS, KV_HEADS, HEAD_DIM), (1, 0, 2))
    head_sinks = sink_logits.reshape(KV_HEADS, group_size)
    query_index = lax.broadcasted_iota(jnp.int32, (WINDOW, 2 * WINDOW), 0)
    key_index = lax.broadcasted_iota(jnp.int32, (WINDOW, 2 * WINDOW), 1)
    distance = WINDOW + query_index - key_index
    in_window = (distance >= 0) & (distance < WINDOW)
    block_start = jnp.arange(block_count, dtype=jnp.int32) * WINDOW - WINDOW
    allowed = in_window[None] & (block_start[:, None, None] + key_index[None] >= 0)

    def banded(rows_in):
        padding = jnp.zeros((WINDOW, HEAD_DIM), rows_in.dtype)
        extended = jnp.concatenate([padding, rows_in], axis=0).reshape(block_count + 1, WINDOW, HEAD_DIM)
        return jnp.concatenate([extended[:-1], extended[1:]], axis=1)

    def one_head(operands):
        group_queries, group_keys, group_values, group_sinks = operands
        blocked = group_queries.reshape(block_count, WINDOW, group_size, HEAD_DIM).astype(jnp.float32)
        scores = jnp.einsum('nqgd,njd->ngqj', blocked, banded(group_keys).astype(jnp.float32)) * HEAD_DIM ** (-0.5)
        scores = jnp.where(allowed[:, None], scores, MASKED_SCORE)
        sink_logit = group_sinks[None, :, None, None]
        row_peak = jnp.maximum(lax.optimization_barrier(jnp.max(scores, axis=-1, keepdims=True)), sink_logit)
        raised = jnp.exp(scores - row_peak)
        denominator = lax.optimization_barrier(jnp.sum(raised, axis=-1, keepdims=True)) + jnp.exp(sink_logit - row_peak)
        weights = (raised / denominator).astype(jnp.bfloat16)
        attended = jnp.einsum('ngqj,njd->nqgd', weights.astype(jnp.float32), banded(group_values).astype(jnp.float32))
        return attended.astype(jnp.bfloat16)
    per_head = lax.map(one_head, (head_queries, head_keys, head_values, head_sinks))
    attended = jnp.transpose(per_head, (1, 2, 0, 3, 4)).reshape(TOKENS, HEADS * HEAD_DIM)
    earlier_rows = jnp.zeros((CONV_WIDTH - 1, CHANNELS), jnp.bfloat16)
    convolved = depthwise(gated_rows, earlier_rows, conv_taps)
    activated = layer_activate(convolved, conv_gain)
    pointwise = jnp.dot(activated, point_weight, preferred_element_type=jnp.float32)
    merged = merge_groups(attended, pointwise, output_gain)
    return jnp.dot(merged, output_weight, preferred_element_type=jnp.float32).astype(jnp.bfloat16)
```

```python
import jax
import jax.numpy as jnp
from jax import lax
from jax.experimental import pallas as pl
from jax.experimental.pallas import tpu as pltpu
from jax.sharding import Mesh
from jax.sharding import PartitionSpec as P

NZ, NX, NC, NY = 8, 4, 2, 4
D = 2048
HEAD_DIM = 64
WINDOW = 128
TAPS = 31
ROWS = 1024
QROWS = 256
LANES = 128
MIX_HALF = 512
SHARD = 16
PART_A = 1280
PART_B = D - PART_A
EPS = 1e-06
NEG = -1e30
F32 = jnp.float32
BF16 = jnp.bfloat16
CHUNKS = (3, 0, 1, 2)
N_REMOTE = 72
N_LOCAL = 24


def kernel(
    tok, gain, wq, wk, wv, sink, wci, wcg, taps, cgain, pw, ogain, ow, out,
    xb, nb, wcat, wkb, wvb, gainb, sinkb, tapb, cgainb, pwb, ogainb, wa, wb,
    qs, kvs, gs, att_s, cv_s, att_r, cv_r, act, merged, ob,
    send_sem, recv_sem, loc_sem,
):
    z = lax.axis_index("z")
    x = lax.axis_index("x")
    c = lax.axis_index("c")
    y = lax.axis_index("y")
    sp = (z * NX + x) * NC + c

    def zr(d):
        return lax.rem(z + (d % NZ), NZ)

    def xr(d):
        return lax.rem(x + (d % NX), NX)

    def yr(d):
        return lax.rem(y + (d % NY), NY)

    def dev(dz=0, dx=0, dy=0):
        return {"z": zr(dz), "x": xr(dx), "c": c, "y": yr(dy)}

    def at_sp(s):
        return {"z": s // (NX * NC), "x": (s // NC) % NX, "c": s % NC, "y": y}

    sibling = {"z": z, "x": x, "c": 1 - c, "y": y}
    after = at_sp(lax.rem(sp + 1, NZ * NX * NC))
    before = at_sp(lax.rem(sp + NZ * NX * NC - 1, NZ * NX * NC))

    local_count = [0]

    def local(src, dst):
        copy = pltpu.make_async_copy(src, dst, loc_sem.at[local_count[0]])
        local_count[0] += 1
        copy.start()
        return copy

    remote_count = [0]
    sent = []

    def remote(src, dst, to):
        i = remote_count[0]
        remote_count[0] += 1
        copy = pltpu.make_async_remote_copy(
            src_ref=src, dst_ref=dst, send_sem=send_sem.at[i], recv_sem=recv_sem.at[i],
            device_id=to, device_id_type=pl.DeviceIdType.MESH,
        )
        copy.start()
        sent.append(copy)
        return copy

    own_a = local(ow.at[:, 0:PART_A], wa.at[z, x, c])
    own_b = local(ow.at[:, PART_A:D], wb.at[z, x, c])

    def rows_of(chunk):
        return pl.ds(chunk * QROWS, QROWS)

    tok_copies = {}
    first = CHUNKS[0]
    tok_copies[first] = local(tok.at[rows_of(first)], xb.at[rows_of(first)])
    gain_copy = local(gain, gainb)
    w_copies = [
        local(wk, wkb),
        local(wv, wvb),
        local(wq, wcat.at[:, 0:128]),
        local(wci, wcat.at[:, 128:256]),
        local(wcg, wcat.at[:, 256:384]),
    ]
    for chunk in CHUNKS[1:]:
        tok_copies[chunk] = local(tok.at[rows_of(chunk)], xb.at[rows_of(chunk)])
    late = [
        local(sink, sinkb),
        local(taps.at[:, pl.ds(pl.multiple_of(y * LANES, LANES), LANES)], tapb),
        local(cgain, cgainb),
        local(ogain, ogainb),
        local(pw, pwb),
    ]

    barrier = pltpu.get_barrier_semaphore()
    partners = [dev(dz=d) for d in (1, -1, 2, -2)]
    partners += [dev(dx=d) for d in (1, -1, 2)]
    partners += [dev(dy=d) for d in (1, -1, 2)]
    partners += [sibling, after, before]
    for partner in partners:
        pl.semaphore_signal(barrier, inc=1, device_id=partner, device_id_type=pl.DeviceIdType.MESH)
    pl.semaphore_wait(barrier, len(partners))

    def move_a(rz, rx, dz, dx):
        block = wa.at[zr(rz), xr(rx), c]
        return remote(block, block, dev(dz=dz, dx=dx))

    def move_b(rx, dx):
        block = wb.at[z, xr(rx), c]
        return remote(block, block, dev(dx=dx))

    def move_row(rz, dz):
        block = wb.at[zr(rz), :, c]
        return remote(block, block, dev(dz=dz))

    def share_a(rz):
        block = wa.at[zr(rz), :, c]
        return remote(block, block, sibling)

    def share_b(rz):
        block = wb.at[zr(rz), :, c]
        return remote(block, block, sibling)

    gather = {}

    def stage0():
        own_a.wait()
        gather["t1"] = [move_a(0, 0, d, 0) for d in (1, -1, 2, -2)]
        own_b.wait()
        gather["bx"] = [move_b(0, d) for d in (1, -1, 2)]
        gather["ax0"] = [move_a(0, 0, 0, d) for d in (1, -1, 2)]

    def stage1():
        for copy in gather["bx"] + gather["t1"]:
            copy.wait_recv()
        gather["t2"] = [move_a(-2, 0, 1, 0), move_a(2, 0, -1, 0), move_a(-2, 0, 2, 0)]
        gather["r1"] = [move_row(0, d) for d in (1, -1, 2, -2)]
        gather["ax1"] = [move_a(rz, 0, 0, d) for rz in (1, -1, 2, -2) for d in (1, -1, 2)]
        gather["sb0"] = [share_b(0)]

    def stage2():
        for copy in gather["t2"] + gather["r1"] + gather["ax0"]:
            copy.wait_recv()
        gather["r2"] = [move_row(-2, 1), move_row(2, -1), move_row(-2, 2)]
        gather["ax2"] = [move_a(rz, 0, 0, d) for rz in (3, -3, -4) for d in (1, -1, 2)]
        gather["sb1"] = [share_b(rz) for rz in (1, -1, 2, -2)]
        gather["sa0"] = [share_a(0)]

    def stage3():
        for copy in gather["ax1"]:
            copy.wait_recv()
        gather["sa1"] = [share_a(rz) for rz in (1, -1, 2, -2)]

    def stage4():
        for copy in gather["r2"] + gather["ax2"]:
            copy.wait_recv()
        gather["sb2"] = [share_b(rz) for rz in (3, -3, -4)]
        gather["sa2"] = [share_a(rz) for rz in (3, -3, -4)]

    stage0()

    def norm(chunk, slot):
        for sub in range(QROWS // 16):
            wide = xb[pl.ds(chunk * QROWS + sub * 16, 16), :].astype(F32)
            mean = jnp.mean(wide * wide, axis=-1, keepdims=True)
            value = wide * lax.rsqrt(mean + EPS) * gainb[...]
            nb[slot, pl.ds(sub * 16, 16), :] = value.astype(BF16)

    lane = lax.broadcasted_iota(jnp.int32, (QROWS, LANES), 1)
    halves = {}

    def project(chunk, slot):
        return jnp.dot(nb[slot], wcat[...], preferred_element_type=F32)

    def keep(chunk, result):
        query = result[:, 0:128]
        low = jnp.where(lane < HEAD_DIM, query, 0.0).astype(BF16)
        high = jnp.where(lane < HEAD_DIM, pltpu.roll(query, HEAD_DIM, 1), 0.0).astype(BF16)
        for j in range(2):
            block = chunk * 2 + j
            qs[pl.ds(block * 256, 128), :] = low[j * 128 : (j + 1) * 128]
            qs[pl.ds(block * 256 + 128, 128), :] = high[j * 128 : (j + 1) * 128]
        gated = result[:, 128:256] * jax.nn.sigmoid(result[:, 256:384])
        gs[pl.ds(32 + chunk * QROWS, QROWS), :] = gated.astype(BF16).astype(F32)
        kvs[pl.ds(WINDOW + chunk * QROWS, QROWS), :] = result[:, 384:512].astype(BF16)

    gain_copy.wait()
    tok_copies[first].wait()
    norm(first, 0)
    for copy in w_copies:
        copy.wait()
    wcat[:, 384:512] = jnp.concatenate([wkb[...], wvb[...]], axis=1)
    halo = []
    for i, chunk in enumerate(CHUNKS):
        if i + 1 < len(CHUNKS):
            tok_copies[CHUNKS[i + 1]].wait()
        result = project(chunk, i % 2)
        if i + 1 < len(CHUNKS):
            norm(CHUNKS[i + 1], (i + 1) % 2)
        keep(chunk, result)
        if i == 0:
            halo.append(remote(kvs.at[pl.ds(ROWS, WINDOW)], kvs.at[pl.ds(0, WINDOW)], after))
            halo.append(remote(gs.at[pl.ds(ROWS, 32)], gs.at[pl.ds(0, 32)], after))
        if i == 1:
            stage1()
    for copy in late:
        copy.wait()
    for copy in halo:
        copy.wait_recv()

    @pl.when(sp == 0)
    def _():
        kvs[pl.ds(0, WINDOW), :] = jnp.zeros((WINDOW, LANES), BF16)
        gs[pl.ds(0, 32), :] = jnp.zeros((32, LANES), F32)

    row = lax.broadcasted_iota(jnp.int32, (WINDOW, WINDOW), 0)
    col = lax.broadcasted_iota(jnp.int32, (WINDOW, WINDOW), 1)
    ahead = col - row
    earlier = ahead > 0

    def attend(block, store):
        keys = kvs[pl.ds(pl.multiple_of(block * WINDOW, WINDOW), 2 * WINDOW), :]
        query = qs[pl.ds(pl.multiple_of(block * 256, 256), 256), :]
        scores = lax.dot_general(
            query, keys, (((1,), (1,)), ((), ())), preferred_element_type=F32
        )
        opening = jnp.where(jnp.logical_and(sp == 0, block == 0), 1, 0)
        closed = ahead * opening > 0
        shares = []
        for h in range(2):
            rows = slice(h * 128, (h + 1) * 128)
            both = jnp.where(earlier, scores[rows, 0:128], scores[rows, 128:256]) * HEAD_DIM ** (-0.5)
            both = jnp.where(closed, NEG, both)
            logit = sinkb[h]
            top = jnp.maximum(jnp.max(both, axis=-1, keepdims=True), logit)
            raised = jnp.exp(both - top)
            total = jnp.sum(raised, axis=-1, keepdims=True) + jnp.exp(logit - top)
            weight = raised * (1.0 / total)
            shares.append(
                jnp.concatenate(
                    [jnp.where(earlier, weight, 0.0), jnp.where(earlier, 0.0, weight)], axis=1
                ).astype(BF16)
            )
        mixed = jnp.dot(jnp.concatenate(shares, axis=0), keys, preferred_element_type=F32)
        lane_here = lax.broadcasted_iota(jnp.int32, (WINDOW, LANES), 1)
        joined = jnp.where(lane_here < HEAD_DIM, pltpu.roll(mixed[0:128], HEAD_DIM, 1), mixed[128:256])
        store(joined.astype(BF16))

    def convolve(quarter, store):
        base = quarter * QROWS
        for sub in range(QROWS // 64):
            total = jnp.zeros((64, LANES), F32)
            for k in range(TAPS):
                total = total + tapb[k : k + 1, :].astype(F32) * gs[pl.ds(base + sub * 64 + 2 + k, 64), :]
            store(sub, total.astype(BF16))

    exchange_att = []
    exchange_cv = []
    for step, turn in enumerate((2, 1, -1, 0)):
        quarter = yr(turn)
        for j in range(2):
            def keep_att(value, j=j):
                if turn == 0:
                    att_r[y, j * 128 : (j + 1) * 128, :] = value
                else:
                    att_s[step, j * 128 : (j + 1) * 128, :] = value

            attend(quarter * 2 + j, keep_att)
        if turn != 0:
            exchange_att.append(remote(att_s.at[step], att_r.at[y], dev(dy=turn)))

        def keep_cv(sub, value):
            if turn == 0:
                cv_r[y, sub * 64 : (sub + 1) * 64, :] = value
            else:
                cv_s[step, sub * 64 : (sub + 1) * 64, :] = value

        convolve(quarter, keep_cv)
        if turn != 0:
            exchange_cv.append(remote(cv_s.at[step], cv_r.at[y], dev(dy=turn)))
        if step == 0:
            stage2()
        if step == 2:
            stage3()

    for copy in exchange_att:
        copy.wait_recv()
    for sub in range(QROWS // 32):
        rows = pl.ds(sub * 32, 32)
        pieces = [att_r[j, rows, :].astype(F32) for j in range(NY)]
        square = sum(jnp.sum(p * p, axis=-1, keepdims=True) for p in pieces)
        scale = lax.rsqrt(square * (1.0 / MIX_HALF) + EPS)
        for j in range(NY):
            cols = slice(j * 128, (j + 1) * 128)
            merged[rows, cols] = (pieces[j] * scale * ogainb[:, cols]).astype(BF16)
    for copy in exchange_cv:
        copy.wait_recv()
    for sub in range(QROWS // 32):
        rows = pl.ds(sub * 32, 32)
        pieces = [cv_r[j, rows, :].astype(F32) for j in range(NY)]
        mean = sum(jnp.sum(p, axis=-1, keepdims=True) for p in pieces) * (1.0 / MIX_HALF)
        pieces = [p - mean for p in pieces]
        square = sum(jnp.sum(p * p, axis=-1, keepdims=True) for p in pieces)
        scale = lax.rsqrt(square * (1.0 / MIX_HALF) + EPS)
        for j in range(NY):
            cols = slice(j * 128, (j + 1) * 128)
            scaled = pieces[j] * scale * cgainb[:, cols]
            act[rows, cols] = (scaled * jax.nn.sigmoid(scaled)).astype(BF16)
    point = jnp.dot(act[...], pwb[...], preferred_element_type=F32)
    square = jnp.sum(point * point, axis=-1, keepdims=True)
    scale = lax.rsqrt(square * (1.0 / MIX_HALF) + EPS)
    merged[:, MIX_HALF:] = (point * scale * ogainb[:, MIX_HALF:]).astype(BF16)

    stage4()
    for name in ("sb0", "sb1", "sb2", "sa0", "sa1", "sa2"):
        for copy in gather[name]:
            copy.wait_recv()
    outs = []
    for start in range(0, D, 256):
        if start < PART_A:
            block = wa[:, :, :, :, start : start + 256]
        else:
            block = wb[:, :, :, :, start - PART_A : start - PART_A + 256]
        ob[:, start : start + 256] = jnp.dot(
            merged[...], block.reshape(2 * MIX_HALF, 256), preferred_element_type=F32
        ).astype(BF16)
        if start % 512 == 256:
            cols = pl.ds(start - 256, 512)
            outs.append(local(ob.at[:, cols], out.at[:, cols]))
    for copy in outs:
        copy.wait()
    for copy in sent:
        copy.wait_send()


def on_device(
    tokens, norm_gain, query_weight, key_weight, value_weight, sink_logits, conv_in_weight,
    conv_gate_weight, conv_taps, conv_gain, point_weight, output_gain, output_weight,
):
    anywhere = pl.BlockSpec(memory_space=pl.ANY)
    return pl.pallas_call(
        kernel,
        name="mixer",
        out_shape=jax.ShapeDtypeStruct((QROWS, D), BF16),
        in_specs=[anywhere] * 13,
        out_specs=anywhere,
        scratch_shapes=[
            pltpu.VMEM((ROWS, D), BF16),
            pltpu.VMEM((2, QROWS, D), BF16),
            pltpu.VMEM((D, 512), BF16),
            pltpu.VMEM((D, 64), BF16),
            pltpu.VMEM((D, 64), BF16),
            pltpu.VMEM((1, D), F32),
            pltpu.SMEM((2,), F32),
            pltpu.VMEM((TAPS, LANES), BF16),
            pltpu.VMEM((1, MIX_HALF), F32),
            pltpu.VMEM((MIX_HALF, MIX_HALF), BF16),
            pltpu.VMEM((1, 2 * MIX_HALF), F32),
            pltpu.VMEM((NZ, NX, NC, SHARD, PART_A), BF16),
            pltpu.VMEM((NZ, NX, NC, SHARD, PART_B), BF16),
            pltpu.VMEM((2 * ROWS, LANES), BF16),
            pltpu.VMEM((WINDOW + ROWS, LANES), BF16),
            pltpu.VMEM((32 + ROWS, LANES), F32),
            pltpu.VMEM((NY - 1, QROWS, LANES), BF16),
            pltpu.VMEM((NY - 1, QROWS, LANES), BF16),
            pltpu.VMEM((NY, QROWS, LANES), BF16),
            pltpu.VMEM((NY, QROWS, LANES), BF16),
            pltpu.VMEM((QROWS, MIX_HALF), BF16),
            pltpu.VMEM((QROWS, 2 * MIX_HALF), BF16),
            pltpu.VMEM((QROWS, D), BF16),
            pltpu.SemaphoreType.DMA((N_REMOTE,)),
            pltpu.SemaphoreType.DMA((N_REMOTE,)),
            pltpu.SemaphoreType.DMA((N_LOCAL,)),
        ],
        compiler_params=pltpu.CompilerParams(
            collective_id=0, has_side_effects=True, vmem_limit_bytes=60 * 1024 * 1024
        ),
    )(
        tokens, norm_gain.reshape(1, D), query_weight, key_weight, value_weight, sink_logits,
        conv_in_weight, conv_gate_weight, conv_taps, conv_gain.reshape(1, MIX_HALF), point_weight,
        output_gain.reshape(1, 2 * MIX_HALF), output_weight,
    )


def solution(mesh):
    split = Mesh(mesh.devices.reshape(NZ, NX, NC, NY), ("z", "x", "c", "y"))
    sp = ("z", "x", "c")
    in_specs = (
        P(sp, None), P(), P(None, "y"), P(None, "y"), P(None, "y"), P("y"), P(None, "y"),
        P(None, "y"), P(), P(), P(), P(), P(sp, None),
    )
    return jax.shard_map(
        on_device, mesh=split, in_specs=in_specs, out_specs=P(("z", "x", "c", "y"), None),
        check_vma=False,
    )
```
